32 devices in a mesh: grp: 2 (over x), kv: 4 (over y, core), tp: 4 (over z).
Axes of the slice: x: 2, y: 2, z: 4, core: 2. Of those that a mesh axis runs over, the one named last changes fastest.
Arguments:
- tokens: bfloat16 [64, 4096], P('grp', ('kv', 'tp')), parts along dimension 0, may hold values from -12 to 12
- gain_in: bfloat16 [4096], P(('kv', 'tp')), may hold values from 0.099609375 to 1.8984375
- gate_in: bfloat16 [4096, 11008], P('kv', 'tp'), may hold values from -0.09375 to 0.09375
- up_in: bfloat16 [4096, 11008], P('kv', 'tp'), may hold values from -0.09375 to 0.09375
- down_in: bfloat16 [11008, 4096], P('tp', 'kv'), may hold values from -0.21875 to 0.21875
- gain_mix: bfloat16 [4096], P(('kv', 'tp')), may hold values from 0.099609375 to 1.8984375
- w_query: bfloat16 [4096, 1024], P('kv', 'tp'), may hold values from -0.09375 to 0.09375
- w_key: bfloat16 [4096, 1024], P('kv', 'tp'), may hold values from -0.09375 to 0.09375
- w_value: bfloat16 [4096, 2048], P('kv', 'tp'), may hold values from -0.09375 to 0.09375
- w_gate: bfloat16 [4096, 2048], P('kv', 'tp'), may hold values from -0.09375 to 0.09375
- w_mixout: bfloat16 [2048, 4096], P('tp', 'kv'), may hold values from -0.125 to 0.125
- forget_rate: float32 [8], P('tp'), may hold values from 0.01 to 0.7
- state_in: float32 [64, 8, 128, 256], P(('grp', 'kv'), 'tp'), parts along dimension 0, may hold values from -0.6 to 0.6
- positions: int32 [64], P(('grp', 'kv')), parts along dimension 0, may hold values from 0 to 8191
- gain_out: bfloat16 [4096], P(('kv', 'tp')), may hold values from 0.099609375 to 1.8984375
- gate_out: bfloat16 [4096, 11008], P('kv', 'tp'), may hold values from -0.09375 to 0.09375
- up_out: bfloat16 [4096, 11008], P('kv', 'tp'), may hold values from -0.09375 to 0.09375
- down_out: bfloat16 [11008, 4096], P('tp', 'kv'), may hold values from -0.21875 to 0.21875
Outputs:
- result: bfloat16 [64, 4096], P('grp', ('kv', 'tp')), parts along dimension 0
- new_state: float32 [64, 8, 128, 256], P(('grp', 'kv'), 'tp'), parts along dimension 0
The draws below stay inside these ranges and needn't reach their ends.
There are 2 independent parts, one for each index of `grp`. The reference program is written for one: setup_inputs(seed, part) draws one part's arguments, and reference() takes and returns one part's arrays. A program takes and returns all parts, laid end to end along the dimension named above; an argument that names none is the same for every part. Nothing has to cross between parts.
All inputs are finite; a program needn't handle non-finite values.
Results may differ from the reference program's by a relative error of at most 0.024.
Values may be sent and summed in bfloat16 or wider, within the bound.
A program may use at most 128 MiB of HBM per device.

```python
import math
import jax
import jax.numpy as jnp
from jax import lax

D = 4096
FF = 11008
HEADS = 8
DK = 128
DV = 256
B = 32
HEAD_GROUP = 2
UNIT_GROUP = 2752
N_TP = 4


def draw_tokens(key, part):
    column_scale = jnp.exp(jnp.log(4.0) * jnp.arange(D, dtype=jnp.float32) / D)
    base = jnp.clip(jax.random.normal(jax.random.fold_in(key, 11), (B, D), jnp.float32), -3.0, 3.0)
    return (base * column_scale[None, :]).astype(jnp.bfloat16)


def plant(values, key, low, largest):
    spot = [jax.random.randint(jax.random.fold_in(key, axis), (), 0, length) for axis, length in enumerate(values.shape)]
    longest = values.shape.index(max(values.shape))
    next_to = spot[:longest] + [(spot[longest] + 1) % values.shape[longest]] + spot[longest + 1:]
    return values.at[tuple(spot)].set(low).at[tuple(next_to)].set(largest)


def with_spikes(entries, rng, source, target, blocks, factor):
    def block_of(axis_at):
        return (jnp.arange(entries.shape[axis_at]) // (entries.shape[axis_at] // blocks)).reshape((-1,) + (1,) * (entries.ndim - 1 - axis_at))

    near = jax.random.permutation(rng, blocks)[block_of(target)]
    far = (block_of(target) + blocks // 2) % blocks
    return jnp.where((block_of(source) == near) | (block_of(source) == far), factor * entries, entries)


def levels(own_key, shape, pieces, low, top_value):
    level = 1.0
    for axis_at, blocks in pieces:
        steps = jax.random.uniform(jax.random.fold_in(jax.random.fold_in(own_key, 6), axis_at), (blocks,), jnp.float32, low / len(pieces), top_value / len(pieces))
        level = level * jnp.repeat(jnp.exp(steps), shape[axis_at] // blocks).reshape((-1,) + (1,) * (len(shape) - 1 - axis_at))
    return level


def noise(key, extent, deviation, most, shards=(), kind=jnp.bfloat16):
    level = levels(key, extent, shards, -0.22, 0.18) if shards else 1.0
    array = jax.random.normal(key, extent, jnp.float32) * deviation * level
    return jnp.minimum(jnp.maximum(array, -most), most).astype(kind)


def heavy_noise(key, shape, scale, bound, cuts, heavy, kind=jnp.bfloat16):
    drawn = scale * jax.random.normal(key, shape, jnp.float32)
    if cuts:
        drawn = drawn * levels(key, shape, cuts, -0.22, 0.18)
    return jnp.clip(with_spikes(drawn, jax.random.fold_in(key, 3), *heavy), -bound, bound).astype(kind)


def setup_inputs(seed: int = 0, part: int = 0) -> dict:
    streams_of = jax.random.split(jax.random.key(seed), 19)
    part_splits = jax.random.split(jax.random.fold_in(streams_of[18], part), 19)
    tokens = draw_tokens(jax.random.fold_in(jax.random.fold_in(streams_of[18], part), 71), part)
    gain_in = jnp.clip(1.0 + 0.18 * jax.random.normal(streams_of[1], (D,), jnp.float32), 0.099609375, 1.8984375).astype(jnp.bfloat16)
    gate_in = noise(streams_of[2], (D, FF), D ** -0.5, 0.09375, ((0, 4), (1, 4)))
    up_in = noise(streams_of[3], (D, FF), D ** -0.5, 0.09375, ((0, 4), (1, 4)))
    down_in = heavy_noise(streams_of[4], (FF, D), (FF // 8) ** -0.5, 0.21875, ((0, 4), (1, 4)), (0, 1, 4, 2.0))
    gain_mix = jnp.clip(1.0 + 0.18 * jax.random.normal(streams_of[5], (D,), jnp.float32), 0.099609375, 1.8984375).astype(jnp.bfloat16)
    w_query = noise(streams_of[6], (D, HEADS * DK), D ** -0.5, 0.09375, ((0, 4), (1, 4)))
    w_key = noise(streams_of[7], (D, HEADS * DK), D ** -0.5, 0.09375, ((0, 4), (1, 4)))
    w_value = noise(streams_of[8], (D, HEADS * DV), D ** -0.5, 0.09375, ((0, 4), (1, 4)))
    w_gate = noise(streams_of[9], (D, HEADS * DV), D ** -0.5, 0.09375, ((0, 4), (1, 4)))
    w_mixout = noise(streams_of[10], (HEADS * DV, D), (HEADS * DV) ** -0.5, 0.125, ((0, 4), (1, 4)))
    forget_rate = jnp.clip(jnp.exp(math.log(0.7) - 4.248495 * jax.random.uniform(streams_of[11], (HEADS,), jnp.float32) ** levels(streams_of[11], (HEADS,), ((0, 4),), -0.2, 0.2)), 0.01, 0.7)
    state_in = noise(part_splits[12], (B, HEADS, DK, DV), 0.1, 0.6, ((0, 4), (1, 4)), jnp.float32)
    positions = plant(jax.random.randint(part_splits[13], (B,), 0, 8192), jax.random.fold_in(part_splits[13], 1), 0, 8191).astype(jnp.int32)
    gain_out = jnp.clip(1.0 + 0.18 * jax.random.normal(streams_of[14], (D,), jnp.float32), 0.099609375, 1.8984375).astype(jnp.bfloat16)
    gate_out = noise(streams_of[15], (D, FF), D ** -0.5, 0.09375, ((0, 4), (1, 4)))
    up_out = noise(streams_of[16], (D, FF), D ** -0.5, 0.09375, ((0, 4), (1, 4)))
    down_out = heavy_noise(streams_of[17], (FF, D), (FF // 8) ** -0.5, 0.21875, ((0, 4), (1, 4)), (0, 1, 4, 2.0))
    return dict(tokens=tokens, gain_in=gain_in, gate_in=gate_in, up_in=up_in, down_in=down_in, gain_mix=gain_mix, w_query=w_query, w_key=w_key, w_value=w_value, w_gate=w_gate, w_mixout=w_mixout, forget_rate=forget_rate, state_in=state_in, positions=positions, gain_out=gain_out, gate_out=gate_out, up_out=up_out, down_out=down_out)


epsilon = 1e-06

def group_sum(hidden, w_down):
    grouped = hidden.reshape(B, N_TP, UNIT_GROUP).astype(jnp.float32)
    weights = w_down.reshape(N_TP, UNIT_GROUP, D).astype(jnp.float32)
    partials = jnp.einsum('bgc,gcd->gbd', grouped, weights)
    rounded = lax.optimization_barrier(partials.astype(jnp.bfloat16)).astype(jnp.float32)
    return lax.optimization_barrier(jnp.sum(rounded, axis=0))

def half_mlp(tokens, gain_row, w_gate, w_up, w_down):
    widened = tokens.astype(jnp.float32)
    factor = lax.rsqrt(lax.optimization_barrier(jnp.mean(widened * widened, axis=-1, keepdims=True)) + epsilon)
    normed = (widened * gain_row.astype(jnp.float32)).astype(jnp.bfloat16)
    gate_sum = factor * jnp.dot(normed, w_gate, preferred_element_type=jnp.float32)
    up_sum = factor * jnp.dot(normed, w_up, preferred_element_type=jnp.float32)
    hidden = (jax.nn.silu(gate_sum) * up_sum).astype(jnp.bfloat16)
    lowered = group_sum(hidden, w_down)
    return (widened + 0.5 * lowered).astype(jnp.bfloat16)

def rotate(vectors, positions):
    half_dim = vectors.shape[-1] // 2
    inverse = jnp.power(10000.0, -jnp.arange(half_dim, dtype=jnp.float32) * 2.0 / vectors.shape[-1])
    angles = positions.astype(jnp.float32)[:, None] * inverse[None, :]
    cosine = jnp.cos(angles)[:, None, :]
    sine_part = jnp.sin(angles)[:, None, :]
    first_half = vectors[..., :half_dim]
    second_half = vectors[..., half_dim:]
    return jnp.concatenate([first_half * cosine - second_half * sine_part, first_half * sine_part + second_half * cosine], axis=-1)

def retention_step(normed, factor, w_query, w_key, w_value, w_gate, forget_rate, state_in, positions):
    count_rows = normed.shape[0]

    def project(weight, head_dim):
        product = factor * jnp.dot(normed, weight, preferred_element_type=jnp.float32)
        rounded = lax.optimization_barrier(product.astype(jnp.bfloat16))
        return rounded.astype(jnp.float32).reshape(count_rows, HEADS, head_dim)
    queries = rotate(project(w_query, DK), positions)
    key_rot = rotate(project(w_key, DK), positions) * DK ** (-0.5)
    values_now = project(w_value, DV)
    gates_now = project(w_gate, DV)
    decays = jnp.exp(-forget_rate)
    carried = jnp.einsum('bhd,bhde->bhe', queries, state_in, precision=lax.Precision.HIGHEST)
    present = lax.optimization_barrier(jnp.sum(queries * key_rot, axis=-1, keepdims=True)) * values_now
    retained = present + decays[None, :, None] * carried
    new_state = decays[None, :, None, None] * state_in + key_rot[..., None] * values_now[..., None, :]
    normed_heads = retained * lax.rsqrt(lax.optimization_barrier(jnp.mean(retained * retained, axis=-1, keepdims=True)) + epsilon)
    mixed = (jax.nn.silu(gates_now) * normed_heads).astype(jnp.bfloat16)
    return (mixed.reshape(count_rows, HEADS * DV), new_state)

def reference(tokens, gain_in, gate_in, up_in, down_in, gain_mix, w_query, w_key, w_value, w_gate, w_mixout, forget_rate, state_in, positions, gain_out, gate_out, up_out, down_out):
    after_first = half_mlp(tokens, gain_in, gate_in, up_in, down_in)
    widened = after_first.astype(jnp.float32)
    factor = lax.rsqrt(lax.optimization_barrier(jnp.mean(widened * widened, axis=-1, keepdims=True)) + epsilon)
    normed = (widened * gain_mix.astype(jnp.float32)).astype(jnp.bfloat16)
    mixed, new_state = retention_step(normed, factor, w_query, w_key, w_value, w_gate, forget_rate, state_in, positions)
    grouped = mixed.reshape(B, N_TP, HEAD_GROUP * DV).astype(jnp.float32)
    weights = w_mixout.reshape(N_TP, HEAD_GROUP * DV, D).astype(jnp.float32)
    partials = jnp.einsum('bgc,gcd->gbd', grouped, weights)
    rounded = lax.optimization_barrier(partials.astype(jnp.bfloat16)).astype(jnp.float32)
    second = (widened + lax.optimization_barrier(jnp.sum(rounded, axis=0))).astype(jnp.bfloat16)
    result = half_mlp(second, gain_out, gate_out, up_out, down_out)
    return (result, new_state)
```

```python
import functools
import math

import jax
import jax.numpy as jnp
from jax import lax
from jax.experimental import pallas as pl
from jax.experimental.pallas import tpu as pltpu
from jax.sharding import PartitionSpec as P

D = 4096
DK = 128
DV = 256


epsilon = 1e-06


def rotate(vectors, positions):
    half_dim = vectors.shape[-1] // 2
    inverse = jnp.power(10000.0, -jnp.arange(half_dim, dtype=jnp.float32) * 2.0 / vectors.shape[-1])
    angles = positions.astype(jnp.float32)[:, None] * inverse[None, :]
    cosine = jnp.cos(angles)[:, None, :]
    sine_part = jnp.sin(angles)[:, None, :]
    first_half = vectors[..., :half_dim]
    second_half = vectors[..., half_dim:]
    return jnp.concatenate(
        [
            first_half * cosine - second_half * sine_part,
            first_half * sine_part + second_half * cosine,
        ],
        axis=-1,
    )


def block_rows(tokens, gain_row):
    raw_block, gain_block = (
        lax.all_gather(tokens, "tp", axis=1, tiled=True),
        lax.all_gather(gain_row[None, :], "tp", axis=1, tiled=True),
    )
    wide_block = raw_block.astype(jnp.float32)
    squares = lax.psum(jnp.sum(wide_block * wide_block, axis=1), "kv")
    normed = (wide_block * gain_block.astype(jnp.float32)).astype(jnp.bfloat16)
    return (normed, lax.rsqrt(squares / D + epsilon))


def half_mlp(tokens, gain_row, w_gate, w_up, w_down):
    widened = tokens.astype(jnp.float32)
    normed, factor = block_rows(tokens, gain_row)
    gate_part = jnp.dot(normed, w_gate, preferred_element_type=jnp.float32)
    up_part = jnp.dot(normed, w_up, preferred_element_type=jnp.float32)
    gate_sum, up_sum = (
        lax.psum(gate_part.astype(jnp.bfloat16), "kv").astype(jnp.float32),
        lax.psum(up_part.astype(jnp.bfloat16), "kv").astype(jnp.float32),
    )
    column = factor[:, None]
    hidden = (jax.nn.silu(column * gate_sum) * (column * up_sum)).astype(jnp.bfloat16)
    partial_value = jnp.dot(hidden, w_down, preferred_element_type=jnp.float32)
    lowered = lax.psum_scatter(
        partial_value.astype(jnp.bfloat16), "tp", scatter_dimension=1, tiled=True
    ).astype(jnp.float32)
    return (widened + 0.5 * lowered).astype(jnp.bfloat16)


def on_device(
    tokens,
    gain_in,
    gate_in,
    up_in,
    down_in,
    gain_mix,
    w_query,
    w_key,
    w_value,
    w_gate,
    w_mixout,
    forget_rate,
    state_in,
    positions,
    gain_out,
    gate_out,
    up_out,
    down_out,
):
    after_first = half_mlp(tokens, gain_in, gate_in, up_in, down_in)
    widened = after_first.astype(jnp.float32)
    own_rows = state_in.shape[0]
    normed, factor_all = block_rows(after_first, gain_mix)
    head_count = w_query.shape[1] // DK
    weights = (w_query, w_key, w_value, w_gate)
    projected = lax.psum_scatter(
        jnp.concatenate(
            [jnp.dot(normed, weight, preferred_element_type=jnp.float32) for weight in weights],
            axis=1,
        ).astype(jnp.bfloat16),
        "kv",
        scatter_dimension=0,
        tiled=True,
    ).astype(jnp.float32)
    factor = lax.dynamic_slice_in_dim(factor_all, lax.axis_index("kv") * own_rows, own_rows)[
        :, None
    ]
    rounded = lax.optimization_barrier((factor * projected).astype(jnp.bfloat16))
    scaled = rounded.astype(jnp.float32)
    bounds = [head_count * DK, 2 * head_count * DK, 2 * head_count * DK + head_count * DV]
    sections = jnp.split(scaled, bounds, axis=1)
    queries = rotate(sections[0].reshape(own_rows, head_count, DK), positions)
    key_rot = rotate(sections[1].reshape(own_rows, head_count, DK), positions) * DK ** (-0.5)
    values_now = sections[2].reshape(own_rows, head_count, DV)
    gates_now = sections[3].reshape(own_rows, head_count, DV)
    decays = jnp.exp(-forget_rate)
    carried = jnp.einsum("bhd,bhde->bhe", queries, state_in, precision=lax.Precision.HIGHEST)
    present = jnp.sum(queries * key_rot, axis=-1, keepdims=True) * values_now
    retained = present + decays[None, :, None] * carried
    new_state = (
        decays[None, :, None, None] * state_in + key_rot[..., None] * values_now[..., None, :]
    )
    normed_heads = retained * lax.rsqrt(
        jnp.mean(retained * retained, axis=-1, keepdims=True) + epsilon
    )
    mixed = (
        (jax.nn.silu(gates_now) * normed_heads)
        .astype(jnp.bfloat16)
        .reshape(own_rows, head_count * DV)
    )
    head_terms = jnp.dot(
        lax.all_gather(mixed, "kv", axis=0, tiled=True),
        w_mixout,
        preferred_element_type=jnp.float32,
    )
    mixed_sum = lax.psum_scatter(
        head_terms.astype(jnp.bfloat16), "tp", scatter_dimension=1, tiled=True
    ).astype(jnp.float32)
    second = (widened + mixed_sum).astype(jnp.bfloat16)
    result = half_mlp(second, gain_out, gate_out, up_out, down_out)
    return (result, new_state)


MESH = pl.DeviceIdType.MESH
TILE = 256
CHUNKS = 3


def chunk_bounds(width):
    tiles = max(1, width // TILE)
    count = min(CHUNKS, tiles)
    edges = [tiles * c // count * TILE for c in range(count)] + [width]
    return list(zip(edges[:-1], edges[1:]))


def times_transposed(lhs, rhs):
    return lax.dot_general(
        lhs, rhs, (((1,), (1,)), ((), ())), preferred_element_type=jnp.float32
    )


def ceil_lanes(width):
    return -(-width // 128) * 128


def silu(values):
    return values / (1.0 + jnp.exp(-values))


def sine_pair(angles):
    turns = jnp.floor(angles * (0.5 / math.pi) + 0.5)
    rest = angles - turns * 6.28125
    rest = rest - turns * (2.0 * math.pi - 6.28125)
    square = rest * rest
    cosine = jnp.zeros_like(rest)
    sine = jnp.zeros_like(rest)
    for power in range(9, -1, -1):
        cosine = cosine * square + (-1.0) ** power / math.factorial(2 * power)
        sine = sine * square + (-1.0) ** power / math.factorial(2 * power + 1)
    return cosine, sine * rest


def layer_kernel(
    n_kv,
    n_tp,
    tokens,
    gain_in,
    gain_mix,
    gain_out,
    forget,
    positions,
    gate_in,
    up_in,
    down_in,
    w_query,
    w_key,
    w_value,
    w_gate,
    w_mixout,
    state_in,
    gate_out,
    up_out,
    down_out,
    result,
    new_state,
    gate_v,
    up_v,
    down_v,
    query_v,
    key_v,
    value_v,
    gates_v,
    mixout_v,
    state_v,
    gains_all,
    feat_all,
    sums_send,
    sums_recv,
    hidden_all,
    down_acc,
    proj_send,
    proj_recv,
    mixed_all,
    part_send,
    part_recv,
    load_sem,
    store_sem,
    send_sem,
    recv_sem,
):
    kv, tp = lax.axis_index("kv"), lax.axis_index("tp")
    rows, fb = tokens.shape
    own = rows // n_kv
    blk = fb * n_tp
    ff = gate_in.shape[0]
    ffp = ceil_lanes(ff)
    _, heads, dk, dv = state_in.shape
    chunks = chunk_bounds(ff)
    full = blk * n_kv

    pairs = []
    for first, last in chunks:
        span = pl.ds(first, last - first)
        pairs.append((gate_in.at[span], gate_v.at[0, span]))
        pairs.append((up_in.at[span], up_v.at[0, span]))
    pairs += [
        (down_in, down_v.at[0]),
        (w_query, query_v),
        (w_key, key_v),
        (w_value, value_v),
        (w_gate, gates_v),
        (state_in, state_v),
        (w_mixout, mixout_v),
        (gate_out, gate_v.at[1]),
        (up_out, up_v.at[1]),
        (down_out, down_v.at[1]),
    ]
    loads = [
        pltpu.make_async_copy(source, target, load_sem.at[place])
        for place, (source, target) in enumerate(pairs)
    ]
    for load in loads:
        load.start()
    first_loads, loads = loads[: 2 * len(chunks)], loads[2 * len(chunks) :]

    barrier = pltpu.get_barrier_semaphore()
    for d in range(1, n_kv):
        pl.semaphore_signal(
            barrier, inc=1, device_id={"kv": lax.rem(kv + d, n_kv)}, device_id_type=MESH
        )
    for d in range(1, n_tp):
        pl.semaphore_signal(
            barrier, inc=1, device_id={"tp": lax.rem(tp + d, n_tp)}, device_id_type=MESH
        )

    sent = []

    def exchange(stage, axis, source, target, place=None):
        n, me = (n_kv, kv) if axis == "kv" else (n_tp, tp)
        started = []
        for d in range(1, n):
            peer = lax.rem(me + d, n)
            copy = pltpu.make_async_remote_copy(
                src_ref=source(peer),
                dst_ref=target.at[me] if place is None else place(target),
                send_sem=send_sem.at[stage, d],
                recv_sem=recv_sem.at[stage, d],
                device_id={axis: peer},
                device_id_type=MESH,
            )
            copy.start()
            started.append(copy)
        sent.extend(started)
        return started

    def arrive(copies):
        for copy in copies:
            copy.wait_recv()

    def gathered_sum(send, recv, lanes):
        total = send[kv, :, lanes].astype(jnp.float32)
        for d in range(1, n_kv):
            total += recv[lax.rem(kv + n_kv - d, n_kv), :, lanes].astype(jnp.float32)
        return total

    def put_rows(send, lanes, product):
        for r in range(n_kv):
            send[r, :, lanes] = product[r * own : (r + 1) * own].astype(jnp.bfloat16)

    def put_squares(send, at, feats):
        squares = jnp.sum(feats * feats, axis=1, keepdims=True)
        high = squares.astype(jnp.bfloat16)
        low = squares - high.astype(jnp.float32)
        put_rows(send, pl.ds(at, 128), jnp.broadcast_to(high.astype(jnp.float32), (rows, 128)))
        put_rows(send, pl.ds(at + 128, 128), jnp.broadcast_to(low, (rows, 128)))

    def row_factor(send, recv, at):
        high = gathered_sum(send, recv, pl.ds(at, 128))
        low = gathered_sum(send, recv, pl.ds(at + 128, 128))
        return lax.rsqrt((high + low)[:, :1] / full + epsilon)

    def block(which, gain_at):
        feats = jnp.concatenate(
            [feat_all[which, t].astype(jnp.float32) for t in range(n_tp)], axis=1
        )
        gains = jnp.concatenate([gains_all[t, gain_at : gain_at + 1] for t in range(n_tp)], axis=1)
        return feats, (feats * gains).astype(jnp.bfloat16)

    def down_exchange(stage, which, lhs, weight, halve, residual, base=None):
        copies = []
        for d in list(range(1, n_tp)) + [0]:
            t = lax.rem(tp + d, n_tp)
            lanes = pl.ds(pl.multiple_of(t * fb, 128), fb)
            product = jnp.dot(lhs, weight[:, lanes], preferred_element_type=jnp.float32)
            if base is not None:
                product += base[t]
            part_send[which, t] = product.astype(jnp.bfloat16)
            if d:
                copy = pltpu.make_async_remote_copy(
                    src_ref=part_send.at[which, t],
                    dst_ref=part_recv.at[which, tp],
                    send_sem=send_sem.at[stage, d],
                    recv_sem=recv_sem.at[stage, d],
                    device_id={"tp": t},
                    device_id_type=MESH,
                )
                copy.start()
                copies.append(copy)
        sent.extend(copies)
        total = part_send[which, tp].astype(jnp.float32)
        for d, copy in enumerate(copies, 1):
            copy.wait_recv()
            total += part_recv[which, lax.rem(tp + n_tp - d, n_tp)].astype(jnp.float32)
        return (residual.astype(jnp.float32) + halve * total).astype(jnp.bfloat16)

    def half_block(which, stage, gain_at, weight_waits, down_wait, residual):
        feats, normed = block(2 * which, gain_at)
        send, recv = sums_send.at[which], sums_recv.at[which]
        put_squares(send, 0, feats)
        count = len(chunks)
        going = []
        for c, (first, last) in enumerate(chunks):
            for wait in weight_waits[c]:
                wait.wait()
            padded = ceil_lanes(last - first)
            gate_at = 256 + 2 * first
            up_at = gate_at + padded

            def step(column, width, first=first, gate_at=gate_at, up_at=up_at):
                lines = pl.ds(first + column, width)
                put_rows(
                    send,
                    pl.ds(gate_at + column, width),
                    times_transposed(normed, gate_v[which, lines, :]),
                )
                put_rows(
                    send,
                    pl.ds(up_at + column, width),
                    times_transposed(normed, up_v[which, lines, :]),
                )

            whole = (last - first) // TILE * TILE

            @pl.loop(0, whole // TILE)
            def _(tile):
                step(pl.multiple_of(tile * TILE, TILE), TILE)

            if last - first > whole:
                step(whole, last - first - whole)
            span = pl.ds(0 if c == 0 else gate_at, 2 * padded + (256 if c == 0 else 0))
            going.append(
                exchange(
                    stage + c,
                    "kv",
                    lambda peer: send.at[peer, :, span],
                    recv,
                    lambda target: target.at[kv, :, span],
                )
            )
        spreading = []
        factor = None
        for c, (first, last) in enumerate(chunks):
            arrive(going[c])
            if factor is None:
                factor = row_factor(send, recv, 0)
            width = last - first
            gate_at = 256 + 2 * first
            gate = factor * gathered_sum(send, recv, pl.ds(gate_at, width))
            up = factor * gathered_sum(send, recv, pl.ds(gate_at + ceil_lanes(width), width))
            hidden_all[which, kv, :, first:last] = (silu(gate) * up).astype(jnp.bfloat16)
            span = pl.ds(first, ceil_lanes(width))
            spreading.append(
                exchange(
                    stage + count + c,
                    "kv",
                    lambda peer: hidden_all.at[which, kv, :, span],
                    hidden_all.at[which],
                    lambda target: target.at[kv, :, span],
                )
            )
        down_wait.wait()
        for c, (first, last) in enumerate(chunks):
            arrive(spreading[c])
            hidden = (
                hidden_all[which, :, :, first:last]
                .astype(jnp.float32)
                .reshape(rows, last - first)
                .astype(jnp.bfloat16)
            )
            weight = down_v.at[which, pl.ds(first, last - first)]
            if c < count - 1:
                for t in range(n_tp):
                    product = jnp.dot(
                        hidden, weight[:, t * fb : (t + 1) * fb], preferred_element_type=jnp.float32
                    )
                    down_acc[t] = product if c == 0 else down_acc[t] + product
        return down_exchange(
            stage + 2 * count,
            2 * which,
            hidden,
            weight,
            0.5,
            residual,
            down_acc if count > 1 else None,
        )

    def spread(stage, which):
        arrive(
            exchange(stage, "tp", lambda peer: feat_all.at[which, tp], feat_all.at[which])
        )

    gains_all[tp] = jnp.concatenate(
        [g[...].astype(jnp.float32) for g in (gain_in, gain_mix, gain_out)]
        + [jnp.zeros((5, fb), jnp.float32)],
        axis=0,
    )
    feat_all[0, tp] = tokens[...]
    pl.semaphore_wait(barrier, n_kv + n_tp - 2)
    feature_copies = exchange(0, "tp", lambda peer: feat_all.at[0, tp], feat_all.at[0])
    gain_copies = exchange(1, "tp", lambda peer: gains_all.at[tp], gains_all)
    lane = lax.broadcasted_iota(jnp.int32, (own, dk), 1)
    line = lax.broadcasted_iota(jnp.int32, (own, dk), 0)
    place = jnp.zeros((own, dk), jnp.float32)
    for r in range(own):
        place = jnp.where(line == r, positions[r].astype(jnp.float32), place)
    half = jnp.where(lane < dk // 2, lane, lane - dk // 2).astype(jnp.float32)
    cosine, sine = sine_pair(place * jnp.exp(half * (-2.0 * math.log(10000.0) / dk)))
    sine = jnp.where(lane < dk // 2, -sine, sine)
    arrive(feature_copies)
    arrive(gain_copies)

    after_first = half_block(
        0, 10, 0, [first_loads[2 * c : 2 * c + 2] for c in range(len(chunks))], loads[0], tokens[...]
    )
    feat_all[1, tp] = after_first
    spread(2, 1)

    feats, normed = block(1, 1)
    widths = (heads * dk, heads * dk, heads * dv, heads * dv)
    total_width = sum(widths)
    put_squares(proj_send, total_width, feats)
    start = 0
    for weight, load, width in zip((query_v, key_v, value_v, gates_v), loads[1:5], widths):
        load.wait()
        for column in range(0, width, TILE):
            size = min(TILE, width - column)
            put_rows(
                proj_send,
                pl.ds(start + column, size),
                jnp.dot(
                    normed, weight[:, column : column + size], preferred_element_type=jnp.float32
                ),
            )
        start += width
    arrive(exchange(3, "kv", lambda peer: proj_send.at[peer], proj_recv))
    factor = row_factor(proj_send, proj_recv, total_width)
    projected = (factor * gathered_sum(proj_send, proj_recv, pl.ds(0, total_width))).astype(
        jnp.bfloat16
    ).astype(jnp.float32)
    loads[5].wait()
    kept = []
    for h in range(heads):
        query = projected[:, h * dk : (h + 1) * dk]
        key = projected[:, (heads + h) * dk : (heads + h + 1) * dk]
        at = 2 * heads * dk + h * dv
        value = projected[:, at : at + dv]
        gate = projected[:, at + heads * dv : at + (heads + 1) * dv]
        query = query * cosine + pltpu.roll(query, dk // 2, axis=1) * sine
        key = (key * cosine + pltpu.roll(key, dk // 2, axis=1) * sine) * dk**-0.5
        query_t, key_t = query.T, key.T
        decay = jnp.exp(jnp.full((1, dv), -forget[h], jnp.float32))
        carried = jnp.concatenate(
            [
                jnp.sum(query_t[:, b : b + 1] * state_v[b, h], axis=0, keepdims=True)
                for b in range(own)
            ],
            axis=0,
        )
        retained = jnp.sum(query * key, axis=1, keepdims=True) * value + decay * carried
        scaled = retained * lax.rsqrt(
            jnp.sum(retained * retained, axis=1, keepdims=True) / dv + epsilon
        )
        mixed_all[kv, :, h * dv : (h + 1) * dv] = (silu(gate) * scaled).astype(jnp.bfloat16)
        kept.append((key_t, value, decay))
    mixed_copies = exchange(4, "kv", lambda peer: mixed_all.at[kv], mixed_all)
    for h, (key_t, value, decay) in enumerate(kept):
        for b in range(own):
            state_v[b, h] = decay * state_v[b, h] + key_t[:, b : b + 1] * value[b : b + 1]
    store = pltpu.make_async_copy(state_v, new_state, store_sem)
    store.start()
    arrive(mixed_copies)
    loads[6].wait()
    mixed = mixed_all[...].astype(jnp.float32).reshape(rows, heads * dv).astype(jnp.bfloat16)
    second = down_exchange(5, 1, mixed, mixout_v, 1.0, after_first)
    feat_all[2, tp] = second
    spread(6, 2)

    result[...] = half_block(
        1,
        11 + 2 * len(chunks),
        2,
        [loads[7:9]] + [[]] * (len(chunks) - 1),
        loads[9],
        second,
    )
    store.wait()
    for copy in sent:
        copy.wait_send()


def fused_layer(
    n_kv,
    n_tp,
    tokens,
    gain_in,
    gate_in,
    up_in,
    down_in,
    gain_mix,
    w_query,
    w_key,
    w_value,
    w_gate,
    w_mixout,
    forget_rate,
    state_in,
    positions,
    gain_out,
    gate_out,
    up_out,
    down_out,
):
    rows, fb = tokens.shape
    blk, ff = gate_in.shape
    own, heads, dk, dv = state_in.shape
    ffp = ceil_lanes(ff)
    bf16 = jnp.bfloat16
    proj_width = 2 * heads * (dk + dv) + 256
    n_most = max(n_kv, n_tp)
    vmem = pl.BlockSpec(memory_space=pltpu.VMEM)
    smem = pl.BlockSpec(memory_space=pltpu.SMEM)
    hbm = pl.BlockSpec(memory_space=pl.ANY)
    gate_in, up_in, gate_out, up_out = gate_in.T, up_in.T, gate_out.T, up_out.T
    stages = 12 + 4 * len(chunk_bounds(ff))
    weights = (gate_in, up_in, down_in, w_query, w_key, w_value, w_gate, w_mixout)
    weights += (state_in, gate_out, up_out, down_out)
    return pl.pallas_call(
        functools.partial(layer_kernel, n_kv, n_tp),
        out_shape=(
            jax.ShapeDtypeStruct(tokens.shape, bf16),
            jax.ShapeDtypeStruct(state_in.shape, jnp.float32),
        ),
        in_specs=[vmem] * 4 + [smem] * 2 + [hbm] * len(weights),
        out_specs=(vmem, hbm),
        scratch_shapes=[
            pltpu.VMEM((2, ff, blk), bf16),
            pltpu.VMEM((2, ff, blk), bf16),
            pltpu.VMEM((2,) + down_in.shape, bf16),
            pltpu.VMEM(w_query.shape, bf16),
            pltpu.VMEM(w_key.shape, bf16),
            pltpu.VMEM(w_value.shape, bf16),
            pltpu.VMEM(w_gate.shape, bf16),
            pltpu.VMEM(w_mixout.shape, bf16),
            pltpu.VMEM(state_in.shape, jnp.float32),
            pltpu.VMEM((n_tp, 8, fb), jnp.float32),
            pltpu.VMEM((3, n_tp, rows, fb), bf16),
            pltpu.VMEM((2, n_kv, own, 2 * ffp + 256), bf16),
            pltpu.VMEM((2, n_kv, own, 2 * ffp + 256), bf16),
            pltpu.VMEM((2, n_kv, own, ffp), bf16),
            pltpu.VMEM((n_tp, rows, fb), jnp.float32),
            pltpu.VMEM((n_kv, own, proj_width), bf16),
            pltpu.VMEM((n_kv, own, proj_width), bf16),
            pltpu.VMEM((n_kv, own, heads * dv), bf16),
            pltpu.VMEM((3, n_tp, rows, fb), bf16),
            pltpu.VMEM((3, n_tp, rows, fb), bf16),
            pltpu.SemaphoreType.DMA((10 + 2 * len(chunk_bounds(ff)),)),
            pltpu.SemaphoreType.DMA,
            pltpu.SemaphoreType.DMA((stages, n_most)),
            pltpu.SemaphoreType.DMA((stages, n_most)),
        ],
        compiler_params=pltpu.CompilerParams(
            collective_id=0, has_side_effects=True, vmem_limit_bytes=60 * 2**20
        ),
        name="fused_layer",
    )(
        tokens,
        gain_in[None, :],
        gain_mix[None, :],
        gain_out[None, :],
        forget_rate,
        positions,
        *weights,
    )


def choose(n_kv, n_tp, *arguments):
    tokens, gate_in, state_in = arguments[0], arguments[2], arguments[12]
    aligned = (
        tokens.shape[1] % 128 == 0
        and gate_in.shape[0] % 128 == 0
        and state_in.shape[0] == 8
        and state_in.shape[2] == 128
    )
    if aligned:
        return fused_layer(n_kv, n_tp, *arguments)
    return on_device(*arguments)


def solution(mesh):
    in_specs = (
        P("grp", ("kv", "tp")),
        P(("kv", "tp")),
        P("kv", "tp"),
        P("kv", "tp"),
        P("tp", "kv"),
        P(("kv", "tp")),
        P("kv", "tp"),
        P("kv", "tp"),
        P("kv", "tp"),
        P("kv", "tp"),
        P("tp", "kv"),
        P("tp"),
        P(("grp", "kv"), "tp", None, None),
        P(("grp", "kv")),
        P(("kv", "tp")),
        P("kv", "tp"),
        P("kv", "tp"),
        P("tp", "kv"),
    )
    out_specs = (P("grp", ("kv", "tp")), P(("grp", "kv"), "tp", None, None))
    body = functools.partial(choose, mesh.shape["kv"], mesh.shape["tp"])
    return jax.shard_map(
        body, mesh=mesh, in_specs=in_specs, out_specs=out_specs, check_vma=False
    )
```

```python
import functools
import math

import jax
import jax.numpy as jnp
from jax import lax
from jax.experimental import pallas as pl
from jax.experimental.pallas import tpu as pltpu
from jax.sharding import PartitionSpec as P

D = 4096
DK = 128
DV = 256


epsilon = 1e-06


def rotate(vectors, positions):
    half_dim = vectors.shape[-1] // 2
    inverse = jnp.power(10000.0, -jnp.arange(half_dim, dtype=jnp.float32) * 2.0 / vectors.shape[-1])
    angles = positions.astype(jnp.float32)[:, None] * inverse[None, :]
    cosine = jnp.cos(angles)[:, None, :]
    sine_part = jnp.sin(angles)[:, None, :]
    first_half = vectors[..., :half_dim]
    second_half = vectors[..., half_dim:]
    return jnp.concatenate(
        [
            first_half * cosine - second_half * sine_part,
            first_half * sine_part + second_half * cosine,
        ],
        axis=-1,
    )


def block_rows(tokens, gain_row):
    raw_block, gain_block = (
        lax.all_gather(tokens, "tp", axis=1, tiled=True),
        lax.all_gather(gain_row[None, :], "tp", axis=1, tiled=True),
    )
    wide_block = raw_block.astype(jnp.float32)
    squares = lax.psum(jnp.sum(wide_block * wide_block, axis=1), "kv")
    normed = (wide_block * gain_block.astype(jnp.float32)).astype(jnp.bfloat16)
    return (normed, lax.rsqrt(squares / D + epsilon))


def half_mlp(tokens, gain_row, w_gate, w_up, w_down):
    widened = tokens.astype(jnp.float32)
    normed, factor = block_rows(tokens, gain_row)
    gate_part = jnp.dot(normed, w_gate, preferred_element_type=jnp.float32)
    up_part = jnp.dot(normed, w_up, preferred_element_type=jnp.float32)
    gate_sum, up_sum = (
        lax.psum(gate_part.astype(jnp.bfloat16), "kv").astype(jnp.float32),
        lax.psum(up_part.astype(jnp.bfloat16), "kv").astype(jnp.float32),
    )
    column = factor[:, None]
    hidden = (jax.nn.silu(column * gate_sum) * (column * up_sum)).astype(jnp.bfloat16)
    partial_value = jnp.dot(hidden, w_down, preferred_element_type=jnp.float32)
    lowered = lax.psum_scatter(
        partial_value.astype(jnp.bfloat16), "tp", scatter_dimension=1, tiled=True
    ).astype(jnp.float32)
    return (widened + 0.5 * lowered).astype(jnp.bfloat16)


def on_device(
    tokens,
    gain_in,
    gate_in,
    up_in,
    down_in,
    gain_mix,
    w_query,
    w_key,
    w_value,
    w_gate,
    w_mixout,
    forget_rate,
    state_in,
    positions,
    gain_out,
    gate_out,
    up_out,
    down_out,
):
    after_first = half_mlp(tokens, gain_in, gate_in, up_in, down_in)
    widened = after_first.astype(jnp.float32)
    own_rows = state_in.shape[0]
    normed, factor_all = block_rows(after_first, gain_mix)
    head_count = w_query.shape[1] // DK
    weights = (w_query, w_key, w_value, w_gate)
    projected = lax.psum_scatter(
        jnp.concatenate(
            [jnp.dot(normed, weight, preferred_element_type=jnp.float32) for weight in weights],
            axis=1,
        ).astype(jnp.bfloat16),
        "kv",
        scatter_dimension=0,
        tiled=True,
    ).astype(jnp.float32)
    factor = lax.dynamic_slice_in_dim(factor_all, lax.axis_index("kv") * own_rows, own_rows)[
        :, None
    ]
    rounded = lax.optimization_barrier((factor * projected).astype(jnp.bfloat16))
    scaled = rounded.astype(jnp.float32)
    bounds = [head_count * DK, 2 * head_count * DK, 2 * head_count * DK + head_count * DV]
    sections = jnp.split(scaled, bounds, axis=1)
    queries = rotate(sections[0].reshape(own_rows, head_count, DK), positions)
    key_rot = rotate(sections[1].reshape(own_rows, head_count, DK), positions) * DK ** (-0.5)
    values_now = sections[2].reshape(own_rows, head_count, DV)
    gates_now = sections[3].reshape(own_rows, head_count, DV)
    decays = jnp.exp(-forget_rate)
    carried = jnp.einsum("bhd,bhde->bhe", queries, state_in, precision=lax.Precision.HIGHEST)
    present = jnp.sum(queries * key_rot, axis=-1, keepdims=True) * values_now
    retained = present + decays[None, :, None] * carried
    new_state = (
        decays[None, :, None, None] * state_in + key_rot[..., None] * values_now[..., None, :]
    )
    normed_heads = retained * lax.rsqrt(
        jnp.mean(retained * retained, axis=-1, keepdims=True) + epsilon
    )
    mixed = (
        (jax.nn.silu(gates_now) * normed_heads)
        .astype(jnp.bfloat16)
        .reshape(own_rows, head_count * DV)
    )
    head_terms = jnp.dot(
        lax.all_gather(mixed, "kv", axis=0, tiled=True),
        w_mixout,
        preferred_element_type=jnp.float32,
    )
    mixed_sum = lax.psum_scatter(
        head_terms.astype(jnp.bfloat16), "tp", scatter_dimension=1, tiled=True
    ).astype(jnp.float32)
    second = (widened + mixed_sum).astype(jnp.bfloat16)
    result = half_mlp(second, gain_out, gate_out, up_out, down_out)
    return (result, new_state)


MESH = pl.DeviceIdType.MESH
TILE = 256
CHUNKS = 5


def chunk_bounds(width):
    tiles = max(1, width // TILE)
    count = min(CHUNKS, tiles)
    edges = [tiles * c // count * TILE for c in range(count)] + [width]
    return list(zip(edges[:-1], edges[1:]))


def times_transposed(lhs, rhs):
    return lax.dot_general(
        lhs, rhs, (((1,), (1,)), ((), ())), preferred_element_type=jnp.float32
    )


def ceil_lanes(width):
    return -(-width // 128) * 128


def silu(values):
    return values / (1.0 + jnp.exp(-values))


def sine_pair(angles):
    turns = jnp.floor(angles * (0.5 / math.pi) + 0.5)
    rest = angles - turns * 6.28125
    rest = rest - turns * (2.0 * math.pi - 6.28125)
    square = rest * rest
    cosine = jnp.zeros_like(rest)
    sine = jnp.zeros_like(rest)
    for power in range(9, -1, -1):
        cosine = cosine * square + (-1.0) ** power / math.factorial(2 * power)
        sine = sine * square + (-1.0) ** power / math.factorial(2 * power + 1)
    return cosine, sine * rest


def layer_kernel(
    n_kv,
    n_tp,
    tokens,
    gain_in,
    gain_mix,
    gain_out,
    forget,
    positions,
    gate_in,
    up_in,
    down_in,
    w_query,
    w_key,
    w_value,
    w_gate,
    w_mixout,
    state_in,
    gate_out,
    up_out,
    down_out,
    result,
    new_state,
    gate_v,
    up_v,
    down_v,
    query_v,
    key_v,
    value_v,
    gates_v,
    mixout_v,
    state_v,
    gains_all,
    feat_all,
    sums_send,
    sums_recv,
    hidden_all,
    down_acc,
    proj_send,
    proj_recv,
    mixed_all,
    part_send,
    part_recv,
    load_sem,
    store_sem,
    send_sem,
    recv_sem,
):
    kv, tp = lax.axis_index("kv"), lax.axis_index("tp")
    rows, fb = tokens.shape
    own = rows // n_kv
    blk = fb * n_tp
    ff = gate_in.shape[0]
    ffp = ceil_lanes(ff)
    _, heads, dk, dv = state_in.shape
    chunks = chunk_bounds(ff)
    full = blk * n_kv

    pairs = []
    for first, last in chunks:
        span = pl.ds(first, last - first)
        pairs.append((gate_in.at[span], gate_v.at[0, span]))
        pairs.append((up_in.at[span], up_v.at[0, span]))
    pairs += [
        (down_in, down_v.at[0]),
        (w_query, query_v),
        (w_key, key_v),
        (w_value, value_v),
        (w_gate, gates_v),
        (state_in, state_v),
        (w_mixout, mixout_v),
        (gate_out, gate_v.at[1]),
        (up_out, up_v.at[1]),
        (down_out, down_v.at[1]),
    ]
    loads = [
        pltpu.make_async_copy(source, target, load_sem.at[place])
        for place, (source, target) in enumerate(pairs)
    ]
    for load in loads:
        load.start()
    first_loads, loads = loads[: 2 * len(chunks)], loads[2 * len(chunks) :]

    barrier = pltpu.get_barrier_semaphore()
    for d in range(1, n_kv):
        pl.semaphore_signal(
            barrier, inc=1, device_id={"kv": lax.rem(kv + d, n_kv)}, device_id_type=MESH
        )
    for d in range(1, n_tp):
        pl.semaphore_signal(
            barrier, inc=1, device_id={"tp": lax.rem(tp + d, n_tp)}, device_id_type=MESH
        )

    sent = []

    def exchange(stage, axis, source, target, place=None):
        n, me = (n_kv, kv) if axis == "kv" else (n_tp, tp)
        started = []
        for d in range(1, n):
            peer = lax.rem(me + d, n)
            copy = pltpu.make_async_remote_copy(
                src_ref=source(peer),
                dst_ref=target.at[me] if place is None else place(target),
                send_sem=send_sem.at[stage, d],
                recv_sem=recv_sem.at[stage, d],
                device_id={axis: peer},
                device_id_type=MESH,
            )
            copy.start()
            started.append(copy)
        sent.extend(started)
        return started

    def arrive(copies):
        for copy in copies:
            copy.wait_recv()

    def gathered_sum(send, recv, lanes):
        total = send[kv, :, lanes].astype(jnp.float32)
        for d in range(1, n_kv):
            total += recv[lax.rem(kv + n_kv - d, n_kv), :, lanes].astype(jnp.float32)
        return total

    def put_rows(send, lanes, product):
        for r in range(n_kv):
            send[r, :, lanes] = product[r * own : (r + 1) * own].astype(jnp.bfloat16)

    def put_squares(send, at, feats):
        squares = jnp.sum(feats * feats, axis=1, keepdims=True)
        high = squares.astype(jnp.bfloat16)
        low = squares - high.astype(jnp.float32)
        put_rows(send, pl.ds(at, 128), jnp.broadcast_to(high.astype(jnp.float32), (rows, 128)))
        put_rows(send, pl.ds(at + 128, 128), jnp.broadcast_to(low, (rows, 128)))

    def row_factor(send, recv, at):
        high = gathered_sum(send, recv, pl.ds(at, 128))
        low = gathered_sum(send, recv, pl.ds(at + 128, 128))
        return lax.rsqrt((high + low)[:, :1] / full + epsilon)

    def block(which, gain_at):
        feats = jnp.concatenate(
            [feat_all[which, t].astype(jnp.float32) for t in range(n_tp)], axis=1
        )
        gains = jnp.concatenate([gains_all[t, gain_at : gain_at + 1] for t in range(n_tp)], axis=1)
        return feats, (feats * gains).astype(jnp.bfloat16)

    def down_exchange(stage, which, lhs, weight, halve, residual, base=None):
        copies = []
        for d in list(range(1, n_tp)) + [0]:
            t = lax.rem(tp + d, n_tp)
            lanes = pl.ds(pl.multiple_of(t * fb, 128), fb)
            product = jnp.dot(lhs, weight[:, lanes], preferred_element_type=jnp.float32)
            if base is not None:
                product += base[t]
            part_send[which, t] = product.astype(jnp.bfloat16)
            if d:
                copy = pltpu.make_async_remote_copy(
                    src_ref=part_send.at[which, t],
                    dst_ref=part_recv.at[which, tp],
                    send_sem=send_sem.at[stage, d],
                    recv_sem=recv_sem.at[stage, d],
                    device_id={"tp": t},
                    device_id_type=MESH,
                )
                copy.start()
                copies.append(copy)
        sent.extend(copies)
        total = part_send[which, tp].astype(jnp.float32)
        for d, copy in enumerate(copies, 1):
            copy.wait_recv()
            total += part_recv[which, lax.rem(tp + n_tp - d, n_tp)].astype(jnp.float32)
        return (residual.astype(jnp.float32) + halve * total).astype(jnp.bfloat16)

    def half_block(which, stage, gain_at, weight_waits, down_wait, residual):
        feats, normed = block(2 * which, gain_at)
        send, recv = sums_send.at[which], sums_recv.at[which]
        put_squares(send, 0, feats)
        count = len(chunks)
        going = []
        for c, (first, last) in enumerate(chunks):
            for wait in weight_waits[c]:
                wait.wait()
            padded = ceil_lanes(last - first)
            gate_at = 256 + 2 * first
            up_at = gate_at + padded

            def step(column, width, first=first, gate_at=gate_at, up_at=up_at):
                lines = pl.ds(first + column, width)
                put_rows(
                    send,
                    pl.ds(gate_at + column, width),
                    times_transposed(normed, gate_v[which, lines, :]),
                )
                put_rows(
                    send,
                    pl.ds(up_at + column, width),
                    times_transposed(normed, up_v[which, lines, :]),
                )

            whole = (last - first) // TILE * TILE

            @pl.loop(0, whole // TILE)
            def _(tile):
                step(pl.multiple_of(tile * TILE, TILE), TILE)

            if last - first > whole:
                step(whole, last - first - whole)
            span = pl.ds(0 if c == 0 else gate_at, 2 * padded + (256 if c == 0 else 0))
            going.append(
                exchange(
                    stage + c,
                    "kv",
                    lambda peer: send.at[peer, :, span],
                    recv,
                    lambda target: target.at[kv, :, span],
                )
            )
        spreading = []
        factor = None
        for c, (first, last) in enumerate(chunks):
            arrive(going[c])
            if factor is None:
                factor = row_factor(send, recv, 0)
            width = last - first
            gate_at = 256 + 2 * first
            gate = factor * gathered_sum(send, recv, pl.ds(gate_at, width))
            up = factor * gathered_sum(send, recv, pl.ds(gate_at + ceil_lanes(width), width))
            hidden_all[which, kv, :, first:last] = (silu(gate) * up).astype(jnp.bfloat16)
            span = pl.ds(first, ceil_lanes(width))
            spreading.append(
                exchange(
                    stage + count + c,
                    "kv",
                    lambda peer: hidden_all.at[which, kv, :, span],
                    hidden_all.at[which],
                    lambda target: target.at[kv, :, span],
                )
            )
        down_wait.wait()
        for c, (first, last) in enumerate(chunks):
            arrive(spreading[c])
            hidden = (
                hidden_all[which, :, :, first:last]
                .astype(jnp.float32)
                .reshape(rows, last - first)
                .astype(jnp.bfloat16)
            )
            weight = down_v.at[which, pl.ds(first, last - first)]
            if c < count - 1:
                for t in range(n_tp):
                    product = jnp.dot(
                        hidden, weight[:, t * fb : (t + 1) * fb], preferred_element_type=jnp.float32
                    )
                    down_acc[t] = product if c == 0 else down_acc[t] + product
        return down_exchange(
            stage + 2 * count,
            2 * which,
            hidden,
            weight,
            0.5,
            residual,
            down_acc if count > 1 else None,
        )

    def spread(stage, which):
        arrive(
            exchange(stage, "tp", lambda peer: feat_all.at[which, tp], feat_all.at[which])
        )

    gains_all[tp] = jnp.concatenate(
        [g[...].astype(jnp.float32) for g in (gain_in, gain_mix, gain_out)]
        + [jnp.zeros((5, fb), jnp.float32)],
        axis=0,
    )
    feat_all[0, tp] = tokens[...]
    pl.semaphore_wait(barrier, n_kv + n_tp - 2)
    feature_copies = exchange(0, "tp", lambda peer: feat_all.at[0, tp], feat_all.at[0])
    gain_copies = exchange(1, "tp", lambda peer: gains_all.at[tp], gains_all)
    lane = lax.broadcasted_iota(jnp.int32, (own, dk), 1)
    line = lax.broadcasted_iota(jnp.int32, (own, dk), 0)
    place = jnp.zeros((own, dk), jnp.float32)
    for r in range(own):
        place = jnp.where(line == r, positions[r].astype(jnp.float32), place)
    half = jnp.where(lane < dk // 2, lane, lane - dk // 2).astype(jnp.float32)
    cosine, sine = sine_pair(place * jnp.exp(half * (-2.0 * math.log(10000.0) / dk)))
    sine = jnp.where(lane < dk // 2, -sine, sine)
    arrive(feature_copies)
    arrive(gain_copies)

    after_first = half_block(
        0, 10, 0, [first_loads[2 * c : 2 * c + 2] for c in range(len(chunks))], loads[0], tokens[...]
    )
    feat_all[1, tp] = after_first
    spread(2, 1)

    feats, normed = block(1, 1)
    widths = (heads * dk, heads * dk, heads * dv, heads * dv)
    total_width = sum(widths)
    put_squares(proj_send, total_width, feats)
    start = 0
    for weight, load, width in zip((query_v, key_v, value_v, gates_v), loads[1:5], widths):
        load.wait()
        for column in range(0, width, TILE):
            size = min(TILE, width - column)
            put_rows(
                proj_send,
                pl.ds(start + column, size),
                jnp.dot(
                    normed, weight[:, column : column + size], preferred_element_type=jnp.float32
                ),
            )
        start += width
    arrive(exchange(3, "kv", lambda peer: proj_send.at[peer], proj_recv))
    factor = row_factor(proj_send, proj_recv, total_width)
    projected = (factor * gathered_sum(proj_send, proj_recv, pl.ds(0, total_width))).astype(
        jnp.bfloat16
    ).astype(jnp.float32)
    loads[5].wait()
    kept = []
    for h in range(heads):
        query = projected[:, h * dk : (h + 1) * dk]
        key = projected[:, (heads + h) * dk : (heads + h + 1) * dk]
        at = 2 * heads * dk + h * dv
        value = projected[:, at : at + dv]
        gate = projected[:, at + heads * dv : at + (heads + 1) * dv]
        query = query * cosine + pltpu.roll(query, dk // 2, axis=1) * sine
        key = (key * cosine + pltpu.roll(key, dk // 2, axis=1) * sine) * dk**-0.5
        query_t, key_t = query.T, key.T
        decay = jnp.exp(jnp.full((1, dv), -forget[h], jnp.float32))
        carried = jnp.concatenate(
            [
                jnp.sum(query_t[:, b : b + 1] * state_v[b, h], axis=0, keepdims=True)
                for b in range(own)
            ],
            axis=0,
        )
        retained = jnp.sum(query * key, axis=1, keepdims=True) * value + decay * carried
        scaled = retained * lax.rsqrt(
            jnp.sum(retained * retained, axis=1, keepdims=True) / dv + epsilon
        )
        mixed_all[kv, :, h * dv : (h + 1) * dv] = (silu(gate) * scaled).astype(jnp.bfloat16)
        kept.append((key_t, value, decay))
    mixed_copies = exchange(4, "kv", lambda peer: mixed_all.at[kv], mixed_all)
    for h, (key_t, value, decay) in enumerate(kept):
        for b in range(own):
            state_v[b, h] = decay * state_v[b, h] + key_t[:, b : b + 1] * value[b : b + 1]
    store = pltpu.make_async_copy(state_v, new_state, store_sem)
    store.start()
    arrive(mixed_copies)
    loads[6].wait()
    mixed = mixed_all[...].astype(jnp.float32).reshape(rows, heads * dv).astype(jnp.bfloat16)
    second = down_exchange(5, 1, mixed, mixout_v, 1.0, after_first)
    feat_all[2, tp] = second
    spread(6, 2)

    result[...] = half_block(
        1,
        11 + 2 * len(chunks),
        2,
        [loads[7:9]] + [[]] * (len(chunks) - 1),
        loads[9],
        second,
    )
    store.wait()
    for copy in sent:
        copy.wait_send()


def fused_layer(
    n_kv,
    n_tp,
    tokens,
    gain_in,
    gate_in,
    up_in,
    down_in,
    gain_mix,
    w_query,
    w_key,
    w_value,
    w_gate,
    w_mixout,
    forget_rate,
    state_in,
    positions,
    gain_out,
    gate_out,
    up_out,
    down_out,
):
    rows, fb = tokens.shape
    blk, ff = gate_in.shape
    own, heads, dk, dv = state_in.shape
    ffp = ceil_lanes(ff)
    bf16 = jnp.bfloat16
    proj_width = 2 * heads * (dk + dv) + 256
    n_most = max(n_kv, n_tp)
    vmem = pl.BlockSpec(memory_space=pltpu.VMEM)
    smem = pl.BlockSpec(memory_space=pltpu.SMEM)
    hbm = pl.BlockSpec(memory_space=pl.ANY)
    gate_in, up_in, gate_out, up_out = gate_in.T, up_in.T, gate_out.T, up_out.T
    stages = 12 + 4 * len(chunk_bounds(ff))
    weights = (gate_in, up_in, down_in, w_query, w_key, w_value, w_gate, w_mixout)
    weights += (state_in, gate_out, up_out, down_out)
    return pl.pallas_call(
        functools.partial(layer_kernel, n_kv, n_tp),
        out_shape=(
            jax.ShapeDtypeStruct(tokens.shape, bf16),
            jax.ShapeDtypeStruct(state_in.shape, jnp.float32),
        ),
        in_specs=[vmem] * 4 + [smem] * 2 + [hbm] * len(weights),
        out_specs=(vmem, hbm),
        scratch_shapes=[
            pltpu.VMEM((2, ff, blk), bf16),
            pltpu.VMEM((2, ff, blk), bf16),
            pltpu.VMEM((2,) + down_in.shape, bf16),
            pltpu.VMEM(w_query.shape, bf16),
            pltpu.VMEM(w_key.shape, bf16),
            pltpu.VMEM(w_value.shape, bf16),
            pltpu.VMEM(w_gate.shape, bf16),
            pltpu.VMEM(w_mixout.shape, bf16),
            pltpu.VMEM(state_in.shape, jnp.float32),
            pltpu.VMEM((n_tp, 8, fb), jnp.float32),
            pltpu.VMEM((3, n_tp, rows, fb), bf16),
            pltpu.VMEM((2, n_kv, own, 2 * ffp + 256), bf16),
            pltpu.VMEM((2, n_kv, own, 2 * ffp + 256), bf16),
            pltpu.VMEM((2, n_kv, own, ffp), bf16),
            pltpu.VMEM((n_tp, rows, fb), jnp.float32),
            pltpu.VMEM((n_kv, own, proj_width), bf16),
            pltpu.VMEM((n_kv, own, proj_width), bf16),
            pltpu.VMEM((n_kv, own, heads * dv), bf16),
            pltpu.VMEM((3, n_tp, rows, fb), bf16),
            pltpu.VMEM((3, n_tp, rows, fb), bf16),
            pltpu.SemaphoreType.DMA((10 + 2 * len(chunk_bounds(ff)),)),
            pltpu.SemaphoreType.DMA,
            pltpu.SemaphoreType.DMA((stages, n_most)),
            pltpu.SemaphoreType.DMA((stages, n_most)),
        ],
        compiler_params=pltpu.CompilerParams(
            collective_id=0, has_side_effects=True, vmem_limit_bytes=60 * 2**20
        ),
        name="fused_layer",
    )(
        tokens,
        gain_in[None, :],
        gain_mix[None, :],
        gain_out[None, :],
        forget_rate,
        positions,
        *weights,
    )


def choose(n_kv, n_tp, *arguments):
    tokens, gate_in, state_in = arguments[0], arguments[2], arguments[12]
    aligned = (
        tokens.shape[1] % 128 == 0
        and gate_in.shape[0] % 128 == 0
        and state_in.shape[0] == 8
        and state_in.shape[2] == 128
    )
    if aligned:
        return fused_layer(n_kv, n_tp, *arguments)
    return on_device(*arguments)


def solution(mesh):
    in_specs = (
        P("grp", ("kv", "tp")),
        P(("kv", "tp")),
        P("kv", "tp"),
        P("kv", "tp"),
        P("tp", "kv"),
        P(("kv", "tp")),
        P("kv", "tp"),
        P("kv", "tp"),
        P("kv", "tp"),
        P("kv", "tp"),
        P("tp", "kv"),
        P("tp"),
        P(("grp", "kv"), "tp", None, None),
        P(("grp", "kv")),
        P(("kv", "tp")),
        P("kv", "tp"),
        P("kv", "tp"),
        P("tp", "kv"),
    )
    out_specs = (P("grp", ("kv", "tp")), P(("grp", "kv"), "tp", None, None))
    body = functools.partial(choose, mesh.shape["kv"], mesh.shape["tp"])
    return jax.shard_map(
        body, mesh=mesh, in_specs=in_specs, out_specs=out_specs, check_vma=False
    )
```
